32 devices in a mesh: sp: 8 (over z, y), tp: 4 (over x, core).
Axes of the slice: x: 2, y: 2, z: 4, core: 2. Of those that a mesh axis runs over, the one named last changes fastest.
Arguments:
- query: bfloat16 [2048, 1024], P('sp', 'tp'), may hold values from -12 to 12
- key_rows: bfloat16 [2048, 512], P('sp', 'tp'), may hold values from -8 to 8
- value_rows: bfloat16 [2048, 512], P('sp', 'tp'), may hold values from -16 to 16
- stream: bfloat16 [2048, 2048], P(('sp', 'tp')), may hold values from -6 to 6
- out_weight: bfloat16 [1024, 2048], P('tp'), may hold values from -0.1875 to 0.1875
- norm_gain: float32 [2048], replicated, may hold values from 0.1 to 1.9
- route_ids: int32 [2048, 4], P(('sp', 'tp')), may hold values from 0 to 7, all different within a row; in each aligned block of 64 rows (0 to 63, 64 to 127, ...) at most 64 rows name the same one
- route_weights: float32 [2048, 4], P(('sp', 'tp')), may hold values from 0.1 to 1
- expert_gate: bfloat16 [8, 2048, 384], P('sp'), may hold values from -0.125 to 0.125
- expert_up: bfloat16 [8, 2048, 384], P('sp'), may hold values from -0.125 to 0.125
- expert_down: bfloat16 [8, 384, 2048], P('sp'), may hold values from -0.3125 to 0.3125
- shared_gate: bfloat16 [2048, 384], replicated, may hold values from -0.125 to 0.125
- shared_up: bfloat16 [2048, 384], replicated, may hold values from -0.125 to 0.125
- shared_down: bfloat16 [384, 2048], replicated, may hold values from -0.3125 to 0.3125
Outputs:
- result: bfloat16 [2048, 2048], P(('sp', 'tp'))
The draws below stay inside these ranges and needn't reach their ends.
Inputs may be any that keep to these rules, and one draw needn't show every extreme that they name: `route_ids`: each row names 4 different experts. Within the rows of one device (aligned blocks of 64 rows) no expert is named more than 64 times, and in some blocks one expert is named exactly 64 times.
All inputs are finite; a program needn't handle non-finite values.
Results may differ from the reference program's by a relative error of at most 0.007.
Values may be sent and summed in bfloat16 or wider, within the bound.
A program may use at most 128 MiB of HBM per device.

```python
import math
import jax
import jax.numpy as jnp
import numpy as np
from jax import lax

D = 2048
HEADS = 8
KV_HEADS = 4
HD = 128
FE = 384
SH = 384
TOP_K = 4
KB = 128
TOK_DEV = 256
TOKEN_SLOTS = 2048
EXPERTS = 8
ROWS = 64
CAP = 64
NBLK = 16


anchor_count = 4


tag_amplitude = 12.0


def common_direction(key):
    raw = jax.random.normal(jax.random.fold_in(key, 101), (KV_HEADS, HD), jnp.float32)
    return raw / jnp.sqrt(jnp.sum(raw * raw, axis=1, keepdims=True)) * HD ** 0.25


def anchor_tags(key):
    direction = common_direction(key)
    unit_dir = direction / jnp.sqrt(jnp.sum(direction * direction, axis=1, keepdims=True))
    partition_count = TOKEN_SLOTS // TOK_DEV
    raw = jax.random.normal(jax.random.fold_in(key, 201), (KV_HEADS, partition_count, anchor_count, HD), jnp.float32)
    along = jnp.sum(raw * unit_dir[:, None, None, :], axis=3, keepdims=True)
    raw = raw - along * unit_dir[:, None, None, :]
    return raw / jnp.sqrt(jnp.sum(raw * raw, axis=3, keepdims=True))


def anchor_offsets(key):
    partition_count = TOKEN_SLOTS // TOK_DEV
    return jax.random.randint(jax.random.fold_in(key, 202), (KV_HEADS, partition_count, anchor_count), 0, TOK_DEV)


def draw_query(key, part):
    direction = common_direction(key)
    fast_share = 0.5
    noise = 0.5 * jax.random.normal(jax.random.fold_in(key, 1), (TOKEN_SLOTS, HEADS, HD), jnp.float32)
    fast = jax.random.uniform(jax.random.fold_in(key, 2), (HEADS,), jnp.float32) < fast_share
    level = jnp.where(fast, -math.log(40.0), -math.log(float(TOKEN_SLOTS))) - 0.4
    head_direction = jnp.repeat(direction, HEADS // KV_HEADS, axis=0)
    shard_of = jnp.arange(TOKEN_SLOTS, dtype=jnp.int32) // TOK_DEV
    target_shard = jax.random.randint(jax.random.fold_in(key, 203), (TOKEN_SLOTS, HEADS), 0, jnp.maximum(shard_of, 1)[:, None])
    target_anchor = jax.random.randint(jax.random.fold_in(key, 204), (TOKEN_SLOTS, HEADS), 0, anchor_count)
    kv_index = jnp.arange(HEADS, dtype=jnp.int32) // (HEADS // KV_HEADS)
    tags = anchor_tags(key)
    chosen = tags[kv_index[None, :], target_shard, target_anchor]
    target_score = jax.random.uniform(jax.random.fold_in(key, 205), (TOKEN_SLOTS, HEADS), jnp.float32, 0.0, 3.0)
    strength = (target_score - level[None, :]) * math.sqrt(HD) / tag_amplitude
    strength = jnp.where(shard_of[:, None] > 0, strength, 0.0)
    full = noise + level[None, :, None] * head_direction[None] + strength[:, :, None] * chosen
    return jnp.clip(full, -12.0, 12.0).reshape(TOKEN_SLOTS, HEADS * HD).astype(jnp.bfloat16)


def draw_key_rows(key, part):
    direction = common_direction(key)
    noise = 0.3 * jax.random.normal(jax.random.fold_in(key, 3), (TOKEN_SLOTS, KV_HEADS, HD), jnp.float32)
    partition_count = TOKEN_SLOTS // TOK_DEV
    shift_amount = jax.random.uniform(jax.random.fold_in(key, 4), (partition_count,), jnp.float32, -0.12, 0.12)
    row_scale = 1.0 + jnp.repeat(shift_amount, TOK_DEV)
    breakage_position = jax.random.randint(jax.random.fold_in(key, 5), (6,), 0, TOKEN_SLOTS)
    broken_weight = jnp.any(jnp.arange(TOKEN_SLOTS)[:, None] == breakage_position[None, :], axis=1)
    row_scale = jnp.where(broken_weight, 0.05, row_scale)
    tags = anchor_tags(key)
    shard_start = jnp.arange(partition_count, dtype=jnp.int32) * TOK_DEV
    positions = (shard_start[None, :, None] + anchor_offsets(key)).reshape(-1)
    head_index = jnp.repeat(jnp.arange(KV_HEADS, dtype=jnp.int32), partition_count * anchor_count)
    planted = jnp.zeros((TOKEN_SLOTS, KV_HEADS, HD), jnp.float32).at[positions, head_index].add(tag_amplitude * tags.reshape(-1, HD))
    full = noise + row_scale[:, None, None] * direction[None] + planted
    return jnp.clip(full, -8.0, 8.0).reshape(TOKEN_SLOTS, KV_HEADS * HD).astype(jnp.bfloat16)


def draw_value_rows(key, part):
    partition_count = TOKEN_SLOTS // TOK_DEV
    noise = 2.0 * jax.random.normal(jax.random.fold_in(key, 6), (TOKEN_SLOTS, KV_HEADS * HD), jnp.float32)
    offsets = 0.5 * jax.random.normal(jax.random.fold_in(key, 7), (partition_count, KV_HEADS * HD), jnp.float32)
    full = noise + jnp.repeat(offsets, TOK_DEV, axis=0)
    return jnp.clip(full, -16.0, 16.0).astype(jnp.bfloat16)


def shard_levels(rng, dims, shards, low, largest):
    def one(dim, blocks):
        steps = jax.random.uniform(jax.random.fold_in(jax.random.fold_in(rng, 6), dim), (blocks,), jnp.float32, low / len(shards), largest / len(shards))
        return jnp.repeat(jnp.exp(steps), dims[dim] // blocks).reshape((-1,) + (1,) * (len(dims) - dim - 1))

    factor_of = one(*shards[0])
    for cut in shards[1:]:
        factor_of = factor_of * one(*cut)
    return factor_of


def assign_block(stream_key, own, number, rows, amount, top, most, skew):
    order = jax.random.permutation(stream_key, amount)
    packed, ordinary = portions_of(amount, rows * top, most, skew, True), portions_of(amount, rows * top, most, skew, False)
    places = jnp.arange(amount)

    def named(tallies, turn):
        used = int((tallies > 0).sum())
        fixed = max(1, used // 4)
        shifted = fixed + (places - fixed + turn * (used - fixed)) % max(1, amount - fixed)
        return jnp.zeros((amount,), jnp.int32).at[order[jnp.where(places < fixed, places, shifted)]].set(jnp.asarray(tallies, jnp.int32))

    tallies = jnp.where(number % 4 == 0, named(packed, number // 4), named(ordinary, number - number // 4 - 1))
    mixed = jax.random.permutation(jax.random.fold_in(own, 3), amount)
    donor, sink = mixed[0:amount // 2 * 2:2], mixed[1:amount // 2 * 2:2]
    margin = jnp.minimum(tallies[donor] - 1, most - tallies[sink]) // 2
    margin = jnp.where((donor == order[0]) | (sink == order[0]) | (tallies[sink] == 0), 0, jnp.maximum(margin, 0))
    shifted = jax.random.randint(jax.random.fold_in(own, 4), (amount // 2,), 0, 1 << 20) % (margin + 1)
    tallies = tallies.at[donor].add(-shifted).at[sink].add(shifted)
    members = jnp.searchsorted(jnp.cumsum(tallies), jnp.arange(rows * top), side="right").astype(jnp.int32)
    listing = members.reshape(top, rows).T
    listing = listing[jax.random.permutation(jax.random.fold_in(own, 1), rows)]
    turn = jax.random.randint(jax.random.fold_in(own, 2), (rows, 1), 0, top)
    return jnp.take_along_axis(listing, (jnp.arange(top)[None, :] + turn) % top, axis=1)


def portions_of(number_of, total, limit, skew, full):
    portions = [(1 << 20) // math.isqrt(grade ** skew) + 1 for grade in range(1, number_of + 1)]
    largest = limit if full else min(limit, max(-(-total // number_of), total * portions[0] // sum(portions)))
    least = 1 if total - largest >= number_of - 1 else 0
    holding, surplus = [largest] + [least] * (number_of - 1), total - largest - least * (number_of - 1)
    while surplus > 0:
        free = [i for i in range(1, number_of) if holding[i] < largest] or [i for i in range(1, number_of) if holding[i] < limit]
        pool, budget = sum([portions[i] for i in free]), surplus
        for i in free:
            extra = min(limit - holding[i], max(1, budget * portions[i] // pool), surplus)
            holding[i] = holding[i] + extra
            surplus = surplus - extra
    return np.array(holding)


def centred(rng, shape, spread, reach, pieces=(), kind=jnp.bfloat16):
    values = spread * jax.random.normal(rng, shape, jnp.float32)
    if pieces:
        values = values * shard_levels(rng, shape, pieces, -0.22, 0.18)
    return jnp.clip(values, -reach, reach).astype(kind)


def setup_inputs(seed: int = 0) -> dict:
    key_list = jax.random.split(jax.random.key(seed), 15)
    query = draw_query(jax.random.fold_in(key_list[14], 71), 0)
    key_rows = draw_key_rows(jax.random.fold_in(key_list[14], 71), 0)
    value_rows = draw_value_rows(jax.random.fold_in(key_list[14], 71), 0)
    stream = centred(key_list[3], (TOKEN_SLOTS, D), 1.0, 6.0, ((0, 32),))
    out_weight = centred(key_list[4], (HEADS * HD, D), (HEADS * HD) ** -0.5, 0.1875, ((0, 4),))
    norm_gain = jnp.clip(1.0 + 0.18 * jax.random.normal(key_list[5], (D,), jnp.float32), 0.1, 1.9)
    route_ids_keys = jax.random.split(jax.random.fold_in(key_list[6], 1), TOKEN_SLOTS // ROWS)
    route_ids_turns = jax.random.permutation(jax.random.fold_in(key_list[6], 3), TOKEN_SLOTS // ROWS)
    route_ids = jax.vmap(lambda own, number: assign_block(jax.random.fold_in(key_list[6], 2), own, number, ROWS, EXPERTS, TOP_K, CAP, 2))(route_ids_keys, route_ids_turns).reshape((TOKEN_SLOTS, TOP_K))
    route_weights = jnp.clip(0.1 + 0.9 * jax.random.uniform(key_list[7], (TOKEN_SLOTS, TOP_K), jnp.float32) ** shard_levels(key_list[7], (TOKEN_SLOTS, TOP_K), ((0, 32),), -0.2, 0.2), 0.1, 1.0)
    expert_gate = centred(key_list[8], (EXPERTS, D, FE), D ** -0.5, 0.125, ((0, 8),))
    expert_up = centred(key_list[9], (EXPERTS, D, FE), D ** -0.5, 0.125, ((0, 8),))
    expert_down = centred(key_list[10], (EXPERTS, FE, D), FE ** -0.5, 0.3125, ((0, 8),))
    shared_gate = centred(key_list[11], (D, SH), D ** -0.5, 0.125)
    shared_up = centred(key_list[12], (D, SH), D ** -0.5, 0.125)
    shared_down = centred(key_list[13], (SH, D), SH ** -0.5, 0.3125)
    return {"query": query, "key_rows": key_rows, "value_rows": value_rows, "stream": stream, "out_weight": out_weight, "norm_gain": norm_gain, "route_ids": route_ids, "route_weights": route_weights, "expert_gate": expert_gate, "expert_up": expert_up, "expert_down": expert_down, "shared_gate": shared_gate, "shared_up": shared_up, "shared_down": shared_down}


def soft_plus(values):
    return jnp.maximum(values, 0.0) + jnp.log1p(jnp.exp(-jnp.abs(values)))

def reference(query, key_rows, value_rows, stream, out_weight, norm_gain, route_ids, route_weights, expert_gate, expert_up, expert_down, shared_gate, shared_up, shared_down):
    query_all = query.reshape(TOKEN_SLOTS, HEADS, HD).astype(jnp.float32)
    keys_all = jnp.repeat(key_rows.reshape(TOKEN_SLOTS, KV_HEADS, HD), HEADS // KV_HEADS, axis=1).astype(jnp.float32)
    values_all = jnp.repeat(value_rows.reshape(TOKEN_SLOTS, KV_HEADS, HD), HEADS // KV_HEADS, axis=1).astype(jnp.float32)
    key_pos = jnp.arange(TOKEN_SLOTS, dtype=jnp.int32)

    def attend_block(block_index):
        block_start = (block_index * KB).astype(jnp.int32)
        block_queries = lax.dynamic_slice_in_dim(query_all, block_start, KB, 0)
        logits = jnp.einsum('qhd,shd->hqs', block_queries, keys_all) * (1.0 / math.sqrt(HD))
        query_pos = block_start + jnp.arange(KB, dtype=jnp.int32)
        visible = key_pos[None, :] < query_pos[:, None]
        penalty = soft_plus(logits)
        breaks = jnp.where(visible, -penalty, 0.0)
        between = jnp.cumsum(breaks[:, :, ::-1], axis=2)[:, :, ::-1] - breaks
        weights = jnp.where(visible, jnp.exp(logits - penalty + between), 0.0).astype(jnp.bfloat16)
        mixed = jnp.einsum('hqs,shd->qhd', weights.astype(jnp.float32), values_all)
        return mixed.astype(jnp.bfloat16)
    heads_out = lax.map(attend_block, jnp.arange(NBLK, dtype=jnp.int32)).reshape(TOKEN_SLOTS, HEADS * HD)
    attended = jnp.dot(heads_out, out_weight, preferred_element_type=jnp.float32)
    mid = (stream.astype(jnp.float32) + attended).astype(jnp.bfloat16)
    mid_wide = lax.optimization_barrier(mid).astype(jnp.float32)
    normed = (mid_wide * lax.rsqrt(lax.optimization_barrier(jnp.mean(mid_wide * mid_wide, axis=1, keepdims=True)) + 1e-06) * norm_gain).astype(jnp.bfloat16)
    flat_ids = route_ids.reshape(-1).astype(jnp.int32)
    most_rows = TOKEN_SLOTS // ROWS * CAP
    padded = jnp.concatenate([normed, jnp.zeros((1, D), jnp.bfloat16)], axis=0)

    def one_expert(expert, output_values):
        slot_spots = jnp.nonzero(flat_ids == expert, size=most_rows, fill_value=TOKEN_SLOTS * TOP_K)[0].astype(jnp.int32)
        taken_rows = padded[slot_spots // TOP_K]
        gate_part = jnp.dot(taken_rows, expert_gate[expert], preferred_element_type=jnp.float32)
        up_part = jnp.dot(taken_rows, expert_up[expert], preferred_element_type=jnp.float32)
        hidden = (jax.nn.silu(gate_part) * up_part).astype(jnp.bfloat16)
        produced = jnp.dot(hidden, expert_down[expert], preferred_element_type=jnp.float32).astype(jnp.bfloat16)
        return output_values.at[slot_spots].set(produced)
    output_values = lax.fori_loop(0, EXPERTS, one_expert, jnp.zeros((TOKEN_SLOTS * TOP_K + 1, D), jnp.bfloat16))
    selected_experts = output_values[:TOKEN_SLOTS * TOP_K].astype(jnp.float32).reshape(TOKEN_SLOTS, TOP_K, D)
    routed = lax.optimization_barrier(jnp.sum(selected_experts * route_weights[:, :, None], axis=1))
    shared_hidden = (jax.nn.silu(jnp.dot(normed, shared_gate, preferred_element_type=jnp.float32)) * jnp.dot(normed, shared_up, preferred_element_type=jnp.float32)).astype(jnp.bfloat16)
    shared_out = jnp.dot(shared_hidden, shared_down, preferred_element_type=jnp.float32)
    return (mid_wide + routed + shared_out).astype(jnp.bfloat16)
```

```python
import functools
import math

import jax
import jax.numpy as jnp
from jax import lax
from jax.experimental import pallas as pl
from jax.experimental.pallas import tpu as pltpu
from jax.sharding import PartitionSpec as P

D = 2048
HD = 128
TOP_K = 4
KB = 128


def shifted(value, axis, steps):
    count = lax.axis_size(axis)
    first, last = (max(0, -steps), min(count, count - steps))
    return lax.ppermute(value, axis, [(source, source + steps) for source in range(first, last)])


def soft_plus(values):
    return jnp.maximum(values, 0.0) + jnp.log1p(jnp.exp(-jnp.abs(values)))


def shard_scores(queries, shard_keys, shard_start, query_pos):
    key_count = shard_keys.shape[0]
    keys_split = shard_keys.reshape(key_count, queries.shape[1], queries.shape[3])
    logits = jnp.einsum("tkgd,skd->kgts", queries, keys_split, preferred_element_type=jnp.float32)
    logits = logits * (1.0 / math.sqrt(queries.shape[3]))
    key_pos = shard_start + jnp.arange(key_count, dtype=jnp.int32)
    visible = key_pos[None, :] < query_pos[:, None]
    penalty = soft_plus(logits)
    breaks = jnp.where(visible, -penalty, 0.0)
    return (logits, penalty, breaks, visible)


def grouped(values, block_size):
    full_shape = values.shape
    return values.reshape(full_shape[:-1] + (full_shape[-1] // block_size, block_size))


def later_matrix(length):
    positions = jnp.arange(length)
    return (positions[:, None] > positions[None, :]).astype(jnp.float32)


def later_sum(values, length):
    return jnp.einsum(
        "kgtm,mb->kgtb", values, later_matrix(length), precision=lax.Precision.HIGHEST
    )


def stick_weights(logits, penalty, breaks, visible, carried, block_size):
    inside = jnp.einsum(
        "kgtnj,js->kgtns",
        grouped(breaks, block_size),
        later_matrix(block_size),
        precision=lax.Precision.HIGHEST,
    )
    log_weight = (
        logits - penalty + inside.reshape(breaks.shape) + jnp.repeat(carried, block_size, axis=3)
    )
    return jnp.where(visible, jnp.exp(log_weight), 0.0).astype(jnp.bfloat16)


def add_values(running, weights, shard_values):
    values_split = shard_values.reshape(shard_values.shape[0], running.shape[0], running.shape[3])
    return running + jnp.einsum(
        "kgts,skd->kgtd", weights, values_split, preferred_element_type=jnp.float32
    )


MESH = pl.DeviceIdType.MESH


def experts_kernel(
    count,
    x_ref,
    mid_ref,
    gate_hbm,
    up_hbm,
    down_hbm,
    sgate_hbm,
    sup_hbm,
    sdown_hbm,
    out_ref,
    gate,
    up,
    down,
    sgate,
    sup,
    sdown,
    gathered,
    kept,
    pair_out,
    pair_in,
    line_out,
    line_in,
    load_sem,
    xz_send,
    xz_recv,
    xy_send,
    xy_recv,
    py_send,
    py_recv,
    lz_send,
    lz_recv,
):
    me = lax.axis_index("sp")
    half = count // 2
    rows, width = mid_ref.shape
    place, side = me // 2, me % 2
    partner = me + 1 - 2 * side

    def along(distance):
        return ((place + distance) % half) * 2 + side

    loads = []
    for number, (source, target) in enumerate(
        (
            (sgate_hbm, sgate),
            (sup_hbm, sup),
            (sdown_hbm, sdown),
            (gate_hbm.at[0], gate),
            (up_hbm.at[0], up),
            (down_hbm.at[0], down),
        )
    ):
        load = pltpu.make_async_copy(source, target, load_sem.at[number])
        load.start()
        loads.append(load)

    barrier = pltpu.get_barrier_semaphore()
    pl.semaphore_signal(barrier, inc=1, device_id={"sp": partner}, device_id_type=MESH)
    for distance in range(1, half):
        pl.semaphore_signal(
            barrier, inc=1, device_id={"sp": along(distance)}, device_id_type=MESH
        )
    pl.semaphore_wait(barrier, half)

    def remote(source, target, send, recv, device):
        return pltpu.make_async_remote_copy(
            src_ref=source,
            dst_ref=target,
            send_sem=send,
            recv_sem=recv,
            device_id={"sp": device},
            device_id_type=MESH,
        )

    order = [0]
    low, high = 1, half - 1
    while low <= high:
        order.append(low)
        if high != low:
            order.append(high)
        low, high = low + 1, high - 1

    top, bottom = pl.ds(0, rows), pl.ds(rows, rows)
    across = {
        d: remote(
            x_ref if d == 0 else gathered.at[d, top],
            gathered.at[d, bottom],
            xy_send.at[d],
            xy_recv.at[d],
            partner,
        )
        for d in order
    }
    spread = {
        d: remote(x_ref, gathered.at[d, top], xz_send.at[d], xz_recv.at[d], along(d))
        for d in order[1:]
    }
    back = {
        d: remote(pair_out.at[d], pair_in.at[d], py_send.at[d], py_recv.at[d], partner)
        for d in order
    }
    home = {
        d: remote(line_out.at[d], line_in.at[d], lz_send.at[d], lz_recv.at[d], along(half - d))
        for d in order[1:]
    }
    across[0].start()
    for d in order[1:]:
        spread[d].start()
    gathered[0, 0:rows] = x_ref[...]

    def hidden_of(values, first, second):
        a = jnp.dot(values, first[...], preferred_element_type=jnp.float32)
        b = jnp.dot(values, second[...], preferred_element_type=jnp.float32)
        return (a / (1.0 + jnp.exp(-a)) * b).astype(jnp.bfloat16)

    for load in loads[:3]:
        load.wait()
    shared = hidden_of(x_ref[:, 0:width], sgate, sup)
    kept[half] = mid_ref[...].astype(jnp.float32) + jnp.dot(
        shared, sdown[...], preferred_element_type=jnp.float32
    )
    for load in loads[3:]:
        load.wait()

    def evaluate(d):
        values = gathered[d]
        extra = values[:, width:].astype(jnp.float32)
        lane = lax.broadcasted_iota(jnp.int32, extra.shape, 1)
        mine = (lane == me) | (lane == me + count)
        weight = jnp.sum(jnp.where(mine, extra, 0.0), axis=1, keepdims=True)
        hidden = hidden_of(values[:, 0:width], gate, up)
        produced = jnp.dot(hidden, down[...], preferred_element_type=jnp.float32)
        produced = produced.astype(jnp.bfloat16).astype(jnp.float32) * weight
        pair_out[d] = produced[rows:].astype(jnp.bfloat16)
        back[d].start()
        kept[d] = produced[:rows]

    def combine(d):
        back[d].wait_recv()
        total = kept[d] + pair_in[d].astype(jnp.float32)
        if d == 0:
            kept[half] = kept[half] + total
        else:
            line_out[d] = total.astype(jnp.bfloat16)
            home[d].start()

    for number in range(half + 1):
        if number + 1 < half:
            following = order[number + 1]
            spread[following].wait_recv()
            across[following].start()
        if number < half:
            across[order[number]].wait_recv()
            evaluate(order[number])
        if number >= 1:
            combine(order[number - 1])

    result = kept[half]
    for d in order[1:]:
        home[d].wait_recv()
        result = result + line_in[d].astype(jnp.float32)
    out_ref[...] = result.astype(out_ref.dtype)
    for d in order:
        across[d].wait_send()
        back[d].wait_send()
        if d != 0:
            spread[d].wait_send()
            home[d].wait_send()


def dense_experts(
    normed,
    mid,
    route_ids,
    route_weights,
    expert_gate,
    expert_up,
    expert_down,
    shared_gate,
    shared_up,
    shared_down,
):
    count = lax.axis_size("sp")
    half = count // 2
    rows, width = normed.shape
    extra = 128 * -(-2 * count // 128)
    named = route_ids[:, :, None] == jnp.arange(count, dtype=jnp.int32)[None, None, :]
    gates = jnp.sum(jnp.where(named, route_weights[:, :, None], 0.0), axis=1)
    coarse = lax.reduce_precision(gates, 8, 7)
    pieces = jnp.concatenate((coarse, gates - coarse), axis=1).astype(jnp.bfloat16)
    pieces = jnp.pad(pieces, ((0, 0), (0, extra - 2 * count)))
    extended = jnp.concatenate((normed, pieces), axis=1)
    fe, sh = expert_gate.shape[2], shared_gate.shape[1]
    vmem, anywhere = pl.BlockSpec(memory_space=pltpu.VMEM), pl.BlockSpec(memory_space=pl.ANY)
    bf16 = jnp.bfloat16
    return pl.pallas_call(
        functools.partial(experts_kernel, count),
        out_shape=jax.ShapeDtypeStruct((rows, width), jnp.bfloat16),
        in_specs=[vmem] * 2 + [anywhere] * 6,
        out_specs=vmem,
        scratch_shapes=[
            pltpu.VMEM((width, fe), bf16),
            pltpu.VMEM((width, fe), bf16),
            pltpu.VMEM((fe, width), bf16),
            pltpu.VMEM((width, sh), bf16),
            pltpu.VMEM((width, sh), bf16),
            pltpu.VMEM((sh, width), bf16),
            pltpu.VMEM((half, 2 * rows, width + extra), bf16),
            pltpu.VMEM((half + 1, rows, width), jnp.float32),
            pltpu.VMEM((half, rows, width), bf16),
            pltpu.VMEM((half, rows, width), bf16),
            pltpu.VMEM((half, rows, width), bf16),
            pltpu.VMEM((half, rows, width), bf16),
            pltpu.SemaphoreType.DMA((6,)),
        ]
        + [pltpu.SemaphoreType.DMA((half,))] * 8,
        compiler_params=pltpu.CompilerParams(
            collective_id=1, has_side_effects=True, vmem_limit_bytes=48 * 1024 * 1024
        ),
    )(
        extended,
        mid,
        expert_gate,
        expert_up,
        expert_down,
        shared_gate,
        shared_up,
        shared_down,
    )


def keep_state(current_state):
    return current_state


def per_device(
    query,
    key_rows,
    value_rows,
    stream,
    out_weight,
    norm_gain,
    route_ids,
    route_weights,
    expert_gate,
    expert_up,
    expert_down,
    shared_gate,
    shared_up,
    shared_down,
):
    tok_rows = query.shape[0]
    kv_local = key_rows.shape[1] // HD
    group_size = query.shape[1] // key_rows.shape[1]
    queries = query.reshape(tok_rows, kv_local, group_size, HD)
    device_pos = lax.axis_index("sp")
    offset = device_pos * tok_rows
    query_pos = offset + jnp.arange(tok_rows, dtype=jnp.int32)
    shard_blocks = tok_rows // KB
    zero_mixed = jnp.zeros((kv_local, group_size, tok_rows, HD), jnp.float32)

    def chain_visit(current_state, shard_keys, shard_values, shard_start):
        mixed_sums, carried_total = current_state
        logits, penalty, breaks, visible = shard_scores(queries, shard_keys, shard_start, query_pos)
        block_totals = grouped(breaks, KB).sum(axis=4)
        carried = later_sum(block_totals, shard_blocks) + carried_total[..., None]
        weights = stick_weights(logits, penalty, breaks, visible, carried, KB)
        return (
            add_values(mixed_sums, weights, shard_values),
            carried_total + block_totals.sum(axis=3),
        )

    start_state = chain_visit(
        (zero_mixed, jnp.zeros((kv_local, group_size, tok_rows), jnp.float32)),
        key_rows,
        value_rows,
        offset,
    )
    moving = jnp.stack((key_rows, value_rows))

    def turn(distance, loop_state):
        current, travelling = loop_state
        travelling = shifted(travelling, "sp", 1)

        def evaluate_layer(current_state):
            return chain_visit(
                current_state, travelling[0], travelling[1], offset - distance * tok_rows
            )

        current = lax.cond(distance <= device_pos, evaluate_layer, keep_state, current)
        return (current, travelling)

    mixed_sums = lax.fori_loop(1, lax.axis_size("sp"), turn, (start_state, moving))[0][0]
    heads_out = (
        mixed_sums.astype(jnp.bfloat16)
        .transpose(2, 0, 1, 3)
        .reshape(tok_rows, kv_local * group_size * HD)
    )
    own_rows = stream.shape[0]
    attended = lax.psum_scatter(
        jnp.dot(heads_out, out_weight, preferred_element_type=jnp.float32),
        "tp",
        scatter_dimension=0,
        tiled=True,
    )
    mid = (stream.astype(jnp.float32) + attended).astype(jnp.bfloat16)
    mid_wide = lax.optimization_barrier(mid).astype(jnp.float32)
    normed = (
        mid_wide
        * lax.rsqrt(jnp.mean(mid_wide * mid_wide, axis=1, keepdims=True) + 1e-06)
        * norm_gain
    ).astype(jnp.bfloat16)
    local_experts = expert_gate.shape[0]
    expert_count = lax.axis_size("sp") * local_experts
    capacity = 2 * own_rows * TOP_K // expert_count
    if capacity >= own_rows and local_experts == 1 and expert_count % 2 == 0:
        return dense_experts(
            normed,
            mid,
            route_ids,
            route_weights,
            expert_gate,
            expert_up,
            expert_down,
            shared_gate,
            shared_up,
            shared_down,
        )
    slot_count = expert_count * capacity
    flat_ids = route_ids.reshape(-1)
    membership = (flat_ids[:, None] == jnp.arange(expert_count, dtype=jnp.int32)[None, :]).astype(
        jnp.int32
    )
    before = jnp.cumsum(membership, axis=0) - membership
    slot_rank = jnp.sum(before * membership, axis=1)
    slot_ids = flat_ids * capacity + slot_rank
    placing = jnp.arange(slot_count, dtype=jnp.int32)[:, None] == slot_ids[None, :]
    dispatch = placing.reshape(slot_count, own_rows, TOP_K).any(axis=2).astype(jnp.bfloat16)
    outgoing = jnp.dot(dispatch, normed, preferred_element_type=jnp.float32).astype(jnp.bfloat16)
    outgoing = outgoing.reshape(lax.axis_size("sp"), local_experts, capacity, D)
    arrived = lax.all_to_all(outgoing, "sp", split_axis=0, concat_axis=0, tiled=True)
    gate_part = jnp.einsum(
        "sepd,edf->sepf", arrived, expert_gate, preferred_element_type=jnp.float32
    )
    up_part = jnp.einsum("sepd,edf->sepf", arrived, expert_up, preferred_element_type=jnp.float32)
    hidden = (jax.nn.silu(gate_part) * up_part).astype(jnp.bfloat16)
    produced = jnp.einsum(
        "sepf,efd->sepd", hidden, expert_down, preferred_element_type=jnp.float32
    ).astype(jnp.bfloat16)
    returned = lax.all_to_all(produced, "sp", split_axis=0, concat_axis=0, tiled=True)
    returned = returned.reshape(slot_count, D)
    picking = (slot_ids[:, None] == jnp.arange(slot_count, dtype=jnp.int32)[None, :]).astype(
        jnp.bfloat16
    )
    selected_experts = jnp.dot(picking, returned, preferred_element_type=jnp.float32).reshape(
        own_rows, TOP_K, D
    )
    routed = jnp.sum(selected_experts * route_weights[:, :, None], axis=1)
    shared_hidden = (
        jax.nn.silu(jnp.dot(normed, shared_gate, preferred_element_type=jnp.float32))
        * jnp.dot(normed, shared_up, preferred_element_type=jnp.float32)
    ).astype(jnp.bfloat16)
    shared_out = jnp.dot(shared_hidden, shared_down, preferred_element_type=jnp.float32)
    return (mid_wide + routed + shared_out).astype(jnp.bfloat16)


def solution(mesh):
    in_specs = (
        P("sp", "tp"),
        P("sp", "tp"),
        P("sp", "tp"),
        P(("sp", "tp"), None),
        P("tp", None),
        P(),
        P(("sp", "tp"), None),
        P(("sp", "tp"), None),
        P("sp", None, None),
        P("sp", None, None),
        P("sp", None, None),
        P(),
        P(),
        P(),
    )
    out_specs = P(("sp", "tp"), None)
    return jax.shard_map(
        per_device, mesh=mesh, in_specs=in_specs, out_specs=out_specs, check_vma=False
    )
```

```python
import functools
import math

import jax
import jax.numpy as jnp
from jax import lax
from jax.experimental import pallas as pl
from jax.experimental.pallas import tpu as pltpu
from jax.sharding import PartitionSpec as P

D = 2048
HD = 128
TOP_K = 4
KB = 128


def shifted(value, axis, steps):
    count = lax.axis_size(axis)
    first, last = (max(0, -steps), min(count, count - steps))
    return lax.ppermute(value, axis, [(source, source + steps) for source in range(first, last)])


def soft_plus(values):
    return jnp.maximum(values, 0.0) + jnp.log1p(jnp.exp(-jnp.abs(values)))


def shard_scores(queries, shard_keys, shard_start, query_pos):
    key_count = shard_keys.shape[0]
    keys_split = shard_keys.reshape(key_count, queries.shape[1], queries.shape[3])
    logits = jnp.einsum("tkgd,skd->kgts", queries, keys_split, preferred_element_type=jnp.float32)
    logits = logits * (1.0 / math.sqrt(queries.shape[3]))
    key_pos = shard_start + jnp.arange(key_count, dtype=jnp.int32)
    visible = key_pos[None, :] < query_pos[:, None]
    penalty = soft_plus(logits)
    breaks = jnp.where(visible, -penalty, 0.0)
    return (logits, penalty, breaks, visible)


def grouped(values, block_size):
    full_shape = values.shape
    return values.reshape(full_shape[:-1] + (full_shape[-1] // block_size, block_size))


def later_matrix(length):
    positions = jnp.arange(length)
    return (positions[:, None] > positions[None, :]).astype(jnp.float32)


def later_sum(values, length):
    return jnp.einsum(
        "kgtm,mb->kgtb", values, later_matrix(length), precision=lax.Precision.HIGHEST
    )


def stick_weights(logits, penalty, breaks, visible, carried, block_size):
    inside = jnp.einsum(
        "kgtnj,js->kgtns",
        grouped(breaks, block_size),
        later_matrix(block_size),
        precision=lax.Precision.HIGHEST,
    )
    log_weight = (
        logits - penalty + inside.reshape(breaks.shape) + jnp.repeat(carried, block_size, axis=3)
    )
    return jnp.where(visible, jnp.exp(log_weight), 0.0).astype(jnp.bfloat16)


def add_values(running, weights, shard_values):
    values_split = shard_values.reshape(shard_values.shape[0], running.shape[0], running.shape[3])
    return running + jnp.einsum(
        "kgts,skd->kgtd", weights, values_split, preferred_element_type=jnp.float32
    )


MESH = pl.DeviceIdType.MESH


def experts_kernel(
    count,
    x_ref,
    mid_ref,
    gate_hbm,
    up_hbm,
    down_hbm,
    sgate_hbm,
    sup_hbm,
    sdown_hbm,
    out_ref,
    gate,
    up,
    down,
    sgate,
    sup,
    sdown,
    gathered,
    kept,
    pair_out,
    pair_in,
    line_out,
    line_in,
    load_sem,
    xz_send,
    xz_recv,
    xy_send,
    xy_recv,
    py_send,
    py_recv,
    lz_send,
    lz_recv,
):
    me = lax.axis_index("sp")
    half = count // 2
    rows, width = mid_ref.shape
    place, side = me // 2, me % 2
    partner = me + 1 - 2 * side

    def along(distance):
        return ((place + distance) % half) * 2 + side

    loads = []
    for number, (source, target) in enumerate(
        (
            (sgate_hbm, sgate),
            (sup_hbm, sup),
            (sdown_hbm, sdown),
            (gate_hbm.at[0], gate),
            (up_hbm.at[0], up),
            (down_hbm.at[0], down),
        )
    ):
        load = pltpu.make_async_copy(source, target, load_sem.at[number])
        load.start()
        loads.append(load)

    barrier = pltpu.get_barrier_semaphore()
    pl.semaphore_signal(barrier, inc=1, device_id={"sp": partner}, device_id_type=MESH)
    for distance in range(1, half):
        pl.semaphore_signal(
            barrier, inc=1, device_id={"sp": along(distance)}, device_id_type=MESH
        )
    pl.semaphore_wait(barrier, half)

    def remote(source, target, send, recv, device):
        return pltpu.make_async_remote_copy(
            src_ref=source,
            dst_ref=target,
            send_sem=send,
            recv_sem=recv,
            device_id={"sp": device},
            device_id_type=MESH,
        )

    order = [0]
    low, high = 1, half - 1
    while low <= high:
        order.append(low)
        if high != low:
            order.append(high)
        low, high = low + 1, high - 1

    top, bottom = pl.ds(0, rows), pl.ds(rows, rows)
    across = {
        d: remote(
            x_ref if d == 0 else gathered.at[d, top],
            gathered.at[d, bottom],
            xy_send.at[d],
            xy_recv.at[d],
            partner,
        )
        for d in order
    }
    spread = {
        d: remote(x_ref, gathered.at[d, top], xz_send.at[d], xz_recv.at[d], along(d))
        for d in order[1:]
    }
    back = {
        d: remote(pair_out.at[d], pair_in.at[d], py_send.at[d], py_recv.at[d], partner)
        for d in order
    }
    home = {
        d: remote(line_out.at[d], line_in.at[d], lz_send.at[d], lz_recv.at[d], along(half - d))
        for d in order[1:]
    }
    across[0].start()
    for d in order[1:]:
        spread[d].start()
    gathered[0, 0:rows] = x_ref[...]

    def hidden_of(values, first, second):
        a = jnp.dot(values, first[...], preferred_element_type=jnp.float32)
        b = jnp.dot(values, second[...], preferred_element_type=jnp.float32)
        return (a / (1.0 + jnp.exp(-a)) * b).astype(jnp.bfloat16)

    for load in loads[:3]:
        load.wait()
    shared = hidden_of(x_ref[:, 0:width], sgate, sup)
    kept[half] = mid_ref[...].astype(jnp.float32) + jnp.dot(
        shared, sdown[...], preferred_element_type=jnp.float32
    )
    for load in loads[3:]:
        load.wait()

    def evaluate(d):
        values = gathered[d]
        extra = values[:, width:].astype(jnp.float32)
        lane = lax.broadcasted_iota(jnp.int32, extra.shape, 1)
        mine = (lane == me) | (lane == me + count)
        weight = jnp.sum(jnp.where(mine, extra, 0.0), axis=1, keepdims=True)
        hidden = hidden_of(values[:, 0:width], gate, up)
        produced = jnp.dot(hidden, down[...], preferred_element_type=jnp.float32)
        produced = produced.astype(jnp.bfloat16).astype(jnp.float32) * weight
        pair_out[d] = produced[rows:].astype(jnp.bfloat16)
        back[d].start()
        kept[d] = produced[:rows]

    def combine(d):
        back[d].wait_recv()
        total = kept[d] + pair_in[d].astype(jnp.float32)
        if d == 0:
            kept[half] = kept[half] + total
        else:
            line_out[d] = total.astype(jnp.bfloat16)
            home[d].start()

    for number in range(half + 1):
        if number + 1 < half:
            following = order[number + 1]
            spread[following].wait_recv()
            across[following].start()
        if number < half:
            across[order[number]].wait_recv()
            evaluate(order[number])
        if number >= 1:
            combine(order[number - 1])

    result = kept[half]
    for d in order[1:]:
        home[d].wait_recv()
        result = result + line_in[d].astype(jnp.float32)
    out_ref[...] = result.astype(out_ref.dtype)
    for d in order:
        across[d].wait_send()
        back[d].wait_send()
        if d != 0:
            spread[d].wait_send()
            home[d].wait_send()


def attention_kernel(
    count,
    peers,
    q_ref,
    kv_ref,
    w_hbm,
    stream_ref,
    gain_ref,
    pieces_ref,
    ext_ref,
    mid_ref,
    shards,
    weights,
    later,
    mixed,
    carried,
    leaving,
    heads,
    load_sem,
    line_send,
    line_recv,
    pair_send,
    pair_recv,
    wx_send,
    wx_recv,
    wc_send,
    wc_recv,
    row_send,
    row_recv,
):
    me, lane_pos = lax.axis_index("sp"), lax.axis_index("tp")
    half, chips = count // 2, peers // 2
    place, side = me // 2, me % 2
    partner = me + 1 - 2 * side
    onward, previous = (me + 2) % count, (me + count - 2) % count
    chip, core = lane_pos // 2, lane_pos % 2
    core_mate = lane_pos + 1 - 2 * core
    tokens, own_rows = q_ref.shape[0], stream_ref.shape[0]
    groups = q_ref.shape[1] // HD
    scale = math.log2(math.e) / math.sqrt(HD)

    load = pltpu.make_async_copy(w_hbm, weights.at[lane_pos], load_sem)
    load.start()
    barrier = pltpu.get_barrier_semaphore()
    for device in (partner, onward, previous):
        pl.semaphore_signal(barrier, inc=1, device_id={"sp": device}, device_id_type=MESH)
    for step in range(1, peers):
        pl.semaphore_signal(
            barrier, inc=1, device_id={"tp": (lane_pos + step) % peers}, device_id_type=MESH
        )
    pl.semaphore_wait(barrier, 3 + peers - 1)

    def remote(source, target, send, recv, **device):
        return pltpu.make_async_remote_copy(
            src_ref=source,
            dst_ref=target,
            send_sem=send,
            recv_sem=recv,
            device_id=device,
            device_id_type=MESH,
        )

    def held(d):
        return kv_ref if d == 0 else shards.at[d, side]

    line = {
        d: remote(held(d - 1), shards.at[d, side], line_send.at[d], line_recv.at[d], sp=onward)
        for d in range(1, half)
    }
    pair = {
        d: remote(held(d), shards.at[d, side], pair_send.at[d], pair_recv.at[d], sp=partner)
        for d in range(half)
    }
    chip_copy = {
        step: remote(
            weights.at[lane_pos],
            weights.at[lane_pos],
            wx_send.at[step],
            wx_recv.at[step],
            tp=((chip + step) % chips) * 2 + core,
        )
        for step in range(1, chips)
    }

    def core_copy(step):
        source = ((chip + chips - step) % chips) * 2 + core
        return remote(
            weights.at[source],
            weights.at[source],
            wc_send.at[step],
            wc_recv.at[step],
            tp=core_mate,
        )

    @pl.when(place + 1 < half)
    def _():
        line[1].start()

    @pl.when(side == 0)
    def _():
        pair[0].start()

    load.wait()
    for step in range(1, chips):
        chip_copy[step].start()
    core_copy(0).start()

    row_pos = lax.broadcasted_iota(jnp.int32, (tokens, tokens), 0)
    key_pos = lax.broadcasted_iota(jnp.int32, (tokens, tokens), 1)
    later[...] = (row_pos > key_pos).astype(jnp.float32).astype(jnp.bfloat16)

    def visit(keys, values, diagonal):
        for group in range(groups):
            queries = q_ref[:, group * HD : (group + 1) * HD]
            logits = scale * lax.dot_general(
                queries, keys, (((1,), (1,)), ((), ())), preferred_element_type=jnp.float32
            )
            tail = jnp.log2(1.0 + jnp.exp2(-jnp.abs(logits)))
            penalty = jnp.maximum(logits, 0.0) + tail
            start = jnp.minimum(logits, 0.0) - tail
            if diagonal:
                visible = key_pos < row_pos
                penalty = jnp.where(visible, penalty, 0.0)
            coarse = penalty.astype(jnp.bfloat16)
            fine = (penalty - coarse.astype(jnp.float32)).astype(jnp.bfloat16)
            inside = jnp.dot(coarse, later[...], preferred_element_type=jnp.float32) + jnp.dot(
                fine, later[...], preferred_element_type=jnp.float32
            )
            total = inside[:, 0:1] + penalty[:, 0:1]
            if diagonal:
                stick = jnp.where(visible, jnp.exp2(start - inside), 0.0)
            else:
                stick = jnp.exp2(start - (inside + carried[group][:, 0:1]))
            part = jnp.dot(
                stick.astype(jnp.bfloat16), values, preferred_element_type=jnp.float32
            )
            if diagonal:
                mixed[group] = part
                carried[group] = jnp.broadcast_to(total, (tokens, HD))
            else:
                mixed[group] = mixed[group] + part
                carried[group] = carried[group] + total

    visit(kv_ref[:, 0:HD], kv_ref[:, HD : 2 * HD], True)

    def relay(d):
        @pl.when(place >= d)
        def _():
            line[d].wait_recv()
            pair[d].start()

        if d + 1 < half:

            @pl.when((place >= d) & (place + 1 < half))
            def _():
                line[d + 1].start()

    for d in range(half):
        if d + 1 < half:
            relay(d + 1)
        if d == 0:

            @pl.when(side == 1)
            def _():
                arrival = remote(
                    kv_ref,
                    shards.at[0, 1 - side],
                    pair_send.at[0],
                    pair_recv.at[0],
                    sp=partner,
                )
                arrival.wait_recv()
                visit(shards[0, 0, :, 0:HD], shards[0, 0, :, HD : 2 * HD], False)

        else:

            @pl.when(place >= d)
            def _():
                pair[d].wait_recv()
                for which in (1, 0):
                    visit(shards[d, which, :, 0:HD], shards[d, which, :, HD : 2 * HD], False)

    for group in range(groups):
        leaving[:, group * HD : (group + 1) * HD] = mixed[group].astype(jnp.bfloat16)
    rows_to = {}
    for step in range(1, peers):
        target = (lane_pos + step) % peers
        rows_to[step] = remote(
            leaving.at[pl.ds(pl.multiple_of(target * own_rows, own_rows), own_rows)],
            heads.at[step],
            row_send.at[step],
            row_recv.at[step],
            tp=target,
        )
        rows_to[step].start()
    own = leaving[pl.ds(pl.multiple_of(lane_pos * own_rows, own_rows), own_rows), :]
    total = stream_ref[...].astype(jnp.float32) + jnp.dot(
        own, weights[lane_pos], preferred_element_type=jnp.float32
    )
    for step in range(1, chips):
        chip_copy[step].wait_recv()
        core_copy(step).start()
    for step in range(1, peers):
        rows_to[step].wait_recv()
    for step in range(chips):
        core_copy(step).wait_recv()
    for step in range(1, peers):
        source = (lane_pos + peers - step) % peers
        total = total + jnp.dot(heads[step], weights[source], preferred_element_type=jnp.float32)
    mid = total.astype(jnp.bfloat16)
    mid_ref[...] = mid
    wide = mid.astype(jnp.float32)
    power = jnp.mean(wide * wide, axis=1, keepdims=True)
    width = mid.shape[1]
    ext_ref[:, 0:width] = (wide * lax.rsqrt(power + 1e-06) * gain_ref[...]).astype(jnp.bfloat16)
    ext_ref[:, width:] = pieces_ref[...]

    @pl.when(side == 0)
    def _():
        pair[0].wait_send()

    for d in range(1, half):

        @pl.when(place >= d)
        def _():
            pair[d].wait_send()

        @pl.when((place + 1 >= d) & (place + 1 < half))
        def _():
            line[d].wait_send()

    for step in range(1, chips):
        chip_copy[step].wait_send()
    for step in range(chips):
        core_copy(step).wait_send()
    for step in range(1, peers):
        rows_to[step].wait_send()


def attend(query, key_rows, value_rows, out_weight, stream, norm_gain, pieces):
    count, peers = lax.axis_size("sp"), lax.axis_size("tp")
    half, chips = count // 2, peers // 2
    tokens, own_rows, width = query.shape[0], stream.shape[0], stream.shape[1]
    groups = query.shape[1] // HD
    vmem, anywhere = pl.BlockSpec(memory_space=pltpu.VMEM), pl.BlockSpec(memory_space=pl.ANY)
    bf16 = jnp.bfloat16
    dma = pltpu.SemaphoreType.DMA
    return pl.pallas_call(
        functools.partial(attention_kernel, count, peers),
        out_shape=(
            jax.ShapeDtypeStruct((own_rows, width + pieces.shape[1]), bf16),
            jax.ShapeDtypeStruct((own_rows, width), bf16),
        ),
        in_specs=[vmem, vmem, anywhere, vmem, vmem, vmem],
        out_specs=(vmem, vmem),
        scratch_shapes=[
            pltpu.VMEM((half, 2, tokens, 2 * HD), bf16),
            pltpu.VMEM((peers,) + out_weight.shape, bf16),
            pltpu.VMEM((tokens, tokens), bf16),
            pltpu.VMEM((groups, tokens, HD), jnp.float32),
            pltpu.VMEM((groups, tokens, HD), jnp.float32),
            pltpu.VMEM((tokens, groups * HD), bf16),
            pltpu.VMEM((peers, own_rows, groups * HD), bf16),
            dma,
        ]
        + [dma((half,))] * 4
        + [dma((chips,))] * 4
        + [dma((peers,))] * 2,
        compiler_params=pltpu.CompilerParams(
            collective_id=2, has_side_effects=True, vmem_limit_bytes=40 * 1024 * 1024
        ),
    )(
        query,
        jnp.concatenate((key_rows, value_rows), axis=1),
        out_weight,
        stream,
        norm_gain.reshape(1, width),
        pieces,
    )


def gate_pieces(route_ids, route_weights):
    count = lax.axis_size("sp")
    extra = 128 * -(-2 * count // 128)
    named = route_ids[:, :, None] == jnp.arange(count, dtype=jnp.int32)[None, None, :]
    gates = jnp.sum(jnp.where(named, route_weights[:, :, None], 0.0), axis=1)
    coarse = lax.reduce_precision(gates, 8, 7)
    pieces = jnp.concatenate((coarse, gates - coarse), axis=1).astype(jnp.bfloat16)
    return jnp.pad(pieces, ((0, 0), (0, extra - 2 * count)))


def dense_experts(
    extended, mid, expert_gate, expert_up, expert_down, shared_gate, shared_up, shared_down
):
    count = lax.axis_size("sp")
    half = count // 2
    rows, width = mid.shape
    extra = extended.shape[1] - width
    fe, sh = expert_gate.shape[2], shared_gate.shape[1]
    vmem, anywhere = pl.BlockSpec(memory_space=pltpu.VMEM), pl.BlockSpec(memory_space=pl.ANY)
    bf16 = jnp.bfloat16
    return pl.pallas_call(
        functools.partial(experts_kernel, count),
        out_shape=jax.ShapeDtypeStruct((rows, width), jnp.bfloat16),
        in_specs=[vmem] * 2 + [anywhere] * 6,
        out_specs=vmem,
        scratch_shapes=[
            pltpu.VMEM((width, fe), bf16),
            pltpu.VMEM((width, fe), bf16),
            pltpu.VMEM((fe, width), bf16),
            pltpu.VMEM((width, sh), bf16),
            pltpu.VMEM((width, sh), bf16),
            pltpu.VMEM((sh, width), bf16),
            pltpu.VMEM((half, 2 * rows, width + extra), bf16),
            pltpu.VMEM((half + 1, rows, width), jnp.float32),
            pltpu.VMEM((half, rows, width), bf16),
            pltpu.VMEM((half, rows, width), bf16),
            pltpu.VMEM((half, rows, width), bf16),
            pltpu.VMEM((half, rows, width), bf16),
            pltpu.SemaphoreType.DMA((6,)),
        ]
        + [pltpu.SemaphoreType.DMA((half,))] * 8,
        compiler_params=pltpu.CompilerParams(
            collective_id=1, has_side_effects=True, vmem_limit_bytes=48 * 1024 * 1024
        ),
    )(
        extended,
        mid,
        expert_gate,
        expert_up,
        expert_down,
        shared_gate,
        shared_up,
        shared_down,
    )


def keep_state(current_state):
    return current_state


def per_device(
    query,
    key_rows,
    value_rows,
    stream,
    out_weight,
    norm_gain,
    route_ids,
    route_weights,
    expert_gate,
    expert_up,
    expert_down,
    shared_gate,
    shared_up,
    shared_down,
):
    tok_rows = query.shape[0]
    kv_local = key_rows.shape[1] // HD
    group_size = query.shape[1] // key_rows.shape[1]
    count, peers = lax.axis_size("sp"), lax.axis_size("tp")
    dense = 2 * stream.shape[0] * TOP_K // (count * expert_gate.shape[0]) >= stream.shape[0]
    even = count % 2 == 0 and count >= 4 and peers % 2 == 0
    if dense and even and kv_local == 1 and expert_gate.shape[0] == 1:
        extended, mid = attend(
            query,
            key_rows,
            value_rows,
            out_weight,
            stream,
            norm_gain,
            gate_pieces(route_ids, route_weights),
        )
        return dense_experts(
            extended, mid, expert_gate, expert_up, expert_down, shared_gate, shared_up, shared_down
        )
    queries = query.reshape(tok_rows, kv_local, group_size, HD)
    device_pos = lax.axis_index("sp")
    offset = device_pos * tok_rows
    query_pos = offset + jnp.arange(tok_rows, dtype=jnp.int32)
    shard_blocks = tok_rows // KB
    zero_mixed = jnp.zeros((kv_local, group_size, tok_rows, HD), jnp.float32)

    def chain_visit(current_state, shard_keys, shard_values, shard_start):
        mixed_sums, carried_total = current_state
        logits, penalty, breaks, visible = shard_scores(queries, shard_keys, shard_start, query_pos)
        block_totals = grouped(breaks, KB).sum(axis=4)
        carried = later_sum(block_totals, shard_blocks) + carried_total[..., None]
        weights = stick_weights(logits, penalty, breaks, visible, carried, KB)
        return (
            add_values(mixed_sums, weights, shard_values),
            carried_total + block_totals.sum(axis=3),
        )

    start_state = chain_visit(
        (zero_mixed, jnp.zeros((kv_local, group_size, tok_rows), jnp.float32)),
        key_rows,
        value_rows,
        offset,
    )
    moving = jnp.stack((key_rows, value_rows))

    def turn(distance, loop_state):
        current, travelling = loop_state
        travelling = shifted(travelling, "sp", 1)

        def evaluate_layer(current_state):
            return chain_visit(
                current_state, travelling[0], travelling[1], offset - distance * tok_rows
            )

        current = lax.cond(distance <= device_pos, evaluate_layer, keep_state, current)
        return (current, travelling)

    mixed_sums = lax.fori_loop(1, lax.axis_size("sp"), turn, (start_state, moving))[0][0]
    heads_out = (
        mixed_sums.astype(jnp.bfloat16)
        .transpose(2, 0, 1, 3)
        .reshape(tok_rows, kv_local * group_size * HD)
    )
    own_rows = stream.shape[0]
    attended = lax.psum_scatter(
        jnp.dot(heads_out, out_weight, preferred_element_type=jnp.float32),
        "tp",
        scatter_dimension=0,
        tiled=True,
    )
    mid = (stream.astype(jnp.float32) + attended).astype(jnp.bfloat16)
    mid_wide = lax.optimization_barrier(mid).astype(jnp.float32)
    normed = (
        mid_wide
        * lax.rsqrt(jnp.mean(mid_wide * mid_wide, axis=1, keepdims=True) + 1e-06)
        * norm_gain
    ).astype(jnp.bfloat16)
    local_experts = expert_gate.shape[0]
    expert_count = lax.axis_size("sp") * local_experts
    capacity = 2 * own_rows * TOP_K // expert_count
    slot_count = expert_count * capacity
    flat_ids = route_ids.reshape(-1)
    membership = (flat_ids[:, None] == jnp.arange(expert_count, dtype=jnp.int32)[None, :]).astype(
        jnp.int32
    )
    before = jnp.cumsum(membership, axis=0) - membership
    slot_rank = jnp.sum(before * membership, axis=1)
    slot_ids = flat_ids * capacity + slot_rank
    placing = jnp.arange(slot_count, dtype=jnp.int32)[:, None] == slot_ids[None, :]
    dispatch = placing.reshape(slot_count, own_rows, TOP_K).any(axis=2).astype(jnp.bfloat16)
    outgoing = jnp.dot(dispatch, normed, preferred_element_type=jnp.float32).astype(jnp.bfloat16)
    outgoing = outgoing.reshape(lax.axis_size("sp"), local_experts, capacity, D)
    arrived = lax.all_to_all(outgoing, "sp", split_axis=0, concat_axis=0, tiled=True)
    gate_part = jnp.einsum(
        "sepd,edf->sepf", arrived, expert_gate, preferred_element_type=jnp.float32
    )
    up_part = jnp.einsum("sepd,edf->sepf", arrived, expert_up, preferred_element_type=jnp.float32)
    hidden = (jax.nn.silu(gate_part) * up_part).astype(jnp.bfloat16)
    produced = jnp.einsum(
        "sepf,efd->sepd", hidden, expert_down, preferred_element_type=jnp.float32
    ).astype(jnp.bfloat16)
    returned = lax.all_to_all(produced, "sp", split_axis=0, concat_axis=0, tiled=True)
    returned = returned.reshape(slot_count, D)
    picking = (slot_ids[:, None] == jnp.arange(slot_count, dtype=jnp.int32)[None, :]).astype(
        jnp.bfloat16
    )
    selected_experts = jnp.dot(picking, returned, preferred_element_type=jnp.float32).reshape(
        own_rows, TOP_K, D
    )
    routed = jnp.sum(selected_experts * route_weights[:, :, None], axis=1)
    shared_hidden = (
        jax.nn.silu(jnp.dot(normed, shared_gate, preferred_element_type=jnp.float32))
        * jnp.dot(normed, shared_up, preferred_element_type=jnp.float32)
    ).astype(jnp.bfloat16)
    shared_out = jnp.dot(shared_hidden, shared_down, preferred_element_type=jnp.float32)
    return (mid_wide + routed + shared_out).astype(jnp.bfloat16)


def solution(mesh):
    in_specs = (
        P("sp", "tp"),
        P("sp", "tp"),
        P("sp", "tp"),
        P(("sp", "tp"), None),
        P("tp", None),
        P(),
        P(("sp", "tp"), None),
        P(("sp", "tp"), None),
        P("sp", None, None),
        P("sp", None, None),
        P("sp", None, None),
        P(),
        P(),
        P(),
    )
    out_specs = P(("sp", "tp"), None)
    return jax.shard_map(
        per_device, mesh=mesh, in_specs=in_specs, out_specs=out_specs, check_vma=False
    )
```
